256 devices in a mesh: sp: 16 (over y, x), tp: 16 (over z, core).
Axes of the slice: x: 4, y: 4, z: 8, core: 2. Of those that a mesh axis runs over, the one named last changes fastest.
Arguments:
- queries: bfloat16 [8192, 2048], P('sp', 'tp'), may hold values from -16 to 16
- key_vectors: bfloat16 [8192, 2048], P('sp', 'tp'), may hold values from -4 to 4
- value_vectors: bfloat16 [8192, 2048], P('sp', 'tp'), may hold values from -5 to 5
- forget_totals: float32 [8192, 16], P('sp', 'tp'), may hold values from -1368 to 0, as said below
- head_gain: float32 [2048], P('tp'), may hold values from 0.1 to 1.9
- stream: bfloat16 [8192, 2048], P(('sp', 'tp')), may hold values from -6 to 6
- out_weight: bfloat16 [2048, 2048], replicated, may hold values from -0.125 to 0.125
- norm_gain: float32 [2048], replicated, may hold values from 0.1 to 1.9
- routing: int32 [8192, 2], P(('sp', 'tp')), may hold values from 0 to 15, all different within a row; in each aligned block of 32 rows (0 to 31, 32 to 63, ...) at most 8 rows name the same one
- route_weights: float32 [8192, 2], P(('sp', 'tp')), may hold values from 0.2 to 1
- gate_weight: bfloat16 [16, 2048, 4096], P('sp', None, 'tp'), may hold values from -0.125 to 0.125
- up_weight: bfloat16 [16, 2048, 4096], P('sp', None, 'tp'), may hold values from -0.125 to 0.125
- down_weight: bfloat16 [16, 4096, 2048], P('sp', 'tp'), may hold values from -0.09375 to 0.09375
Outputs:
- layer_out: bfloat16 [8192, 2048], P(('sp', 'tp'))
The draws below stay inside these ranges and needn't reach their ends.
Inputs may be any that keep to these rules, and one draw needn't show every extreme that they name: `forget_totals`: along the positions, the values of each head never rise. `routing`: A token's 2 experts differ. Within the tokens of one device (aligned blocks of 32 rows) no expert is named more than 8 times.
All inputs are finite; a program needn't handle non-finite values.
Results may differ from the reference program's by a relative error of at most 0.01145.
Values may be sent and summed in bfloat16 or wider, within the bound.
A program may use at most 128 MiB of HBM per device.

```python
import math
import jax
import jax.numpy as jnp
import numpy as np
from jax import lax

D = 2048
HEAD_COUNT = 16
HD = 128
FF_E = 4096
TOP = 2
TOK_DEV = 512
SEQUENCE_TOKENS = 8192
EXPERTS = 16
ROWS_DEV = 32
CAP = 8
N_TP = 16


def draw_queries(key, part):
    own_key = jax.random.fold_in(key, 11)
    entries = jnp.clip(jax.random.normal(own_key, (SEQUENCE_TOKENS, HEAD_COUNT * HD), jnp.float32), -4.0, 4.0)
    return entries.astype(jnp.bfloat16)


def draw_key_vectors(key, part):
    own_key = jax.random.fold_in(key, 13)
    entries = jnp.clip(jax.random.normal(own_key, (SEQUENCE_TOKENS, HEAD_COUNT * HD), jnp.float32), -4.0, 4.0)
    return entries.astype(jnp.bfloat16)


def draw_forget_totals(key, part):
    ranking = jax.random.permutation(jax.random.fold_in(key, 21), HEAD_COUNT)
    slow_heads = ranking < HEAD_COUNT // 2
    slow_rate = jax.random.uniform(jax.random.fold_in(key, 22), (HEAD_COUNT,), jnp.float32, 0.3, 0.8) / SEQUENCE_TOKENS
    fast_rate = jnp.exp(-jax.random.uniform(jax.random.fold_in(key, 23), (HEAD_COUNT,), jnp.float32, math.log(30.0), math.log(100.0)))
    head_rate = jnp.where(slow_heads, slow_rate, fast_rate)
    block_factor = jnp.exp(jax.random.uniform(jax.random.fold_in(key, 24), (SEQUENCE_TOKENS // TOK_DEV, HEAD_COUNT), jnp.float32, math.log(0.5), math.log(1.5)))
    block_factor = jnp.repeat(block_factor, TOK_DEV, axis=0)
    step_factor = jnp.exp(jax.random.uniform(jax.random.fold_in(key, 25), (SEQUENCE_TOKENS, HEAD_COUNT), jnp.float32, math.log(0.3), math.log(3.0)))
    gate_logarithms = -head_rate[None, :] * block_factor * step_factor
    cluster_positions = jax.random.randint(jax.random.fold_in(key, 26), (3,), 0, SEQUENCE_TOKENS)
    cluster_sizes = jnp.log(jax.random.uniform(jax.random.fold_in(key, 27), (3, HEAD_COUNT), jnp.float32, 0.5, 0.8))
    gate_logarithms = gate_logarithms.at[cluster_positions].add(cluster_sizes)
    return jnp.cumsum(gate_logarithms, axis=0).astype(jnp.float32)


def block_scale(key, dims, shards, least, largest):
    gain = 1.0
    for axis_at, blocks in shards:
        steps = jax.random.uniform(jax.random.fold_in(jax.random.fold_in(key, 6), axis_at), (blocks,), jnp.float32, least / len(shards), largest / len(shards))
        gain = gain * jnp.repeat(jnp.exp(steps), dims[axis_at] // blocks).reshape((-1,) + (1,) * (len(dims) - 1 - axis_at))
    return gain


def routed_block(stream_key, own, number, rows, amount, top, bound, skew):
    sequence = jax.random.permutation(stream_key, amount)
    heavy_load, usual = portions_of(amount, rows * top, bound, skew, True), portions_of(amount, rows * top, bound, skew, False)
    places = jnp.arange(amount)

    def named(lengths, rotation):
        used = int((lengths > 0).sum())
        fixed = max(1, used // 4)
        shifted = fixed + (places - fixed + rotation * (used - fixed)) % max(1, amount - fixed)
        return jnp.zeros((amount,), jnp.int32).at[sequence[jnp.where(places < fixed, places, shifted)]].set(jnp.asarray(lengths, jnp.int32))

    lengths = jnp.where(number % 4 == 0, named(heavy_load, number // 4), named(usual, number - number // 4 - 1))
    mixed = jax.random.permutation(jax.random.fold_in(own, 3), amount)
    donor, receiver = mixed[0:amount // 2 * 2:2], mixed[1:amount // 2 * 2:2]
    slack = jnp.minimum(lengths[donor] - 1, bound - lengths[receiver]) // 2
    slack = jnp.where((donor == sequence[0]) | (receiver == sequence[0]) | (lengths[receiver] == 0), 0, jnp.maximum(slack, 0))
    shifted = jax.random.randint(jax.random.fold_in(own, 4), (amount // 2,), 0, 1 << 20) % (slack + 1)
    lengths = lengths.at[donor].add(-shifted).at[receiver].add(shifted)
    labels = jnp.searchsorted(jnp.cumsum(lengths), jnp.arange(rows * top), side="right").astype(jnp.int32)
    table = labels.reshape(top, rows).T
    table = table[jax.random.permutation(jax.random.fold_in(own, 1), rows)]
    rotation = jax.random.randint(jax.random.fold_in(own, 2), (rows, 1), 0, top)
    return jnp.take_along_axis(table, (jnp.arange(top)[None, :] + rotation) % top, axis=1)


def portions_of(number_of, total, most, slope, full):
    weights = [(1 << 20) // math.isqrt(rank ** slope) + 1 for rank in range(1, number_of + 1)]
    largest = most if full else min(most, max(-(-total // number_of), total * weights[0] // sum(weights)))
    least = 1 if total - largest >= number_of - 1 else 0
    given, spare = [largest] + [least] * (number_of - 1), total - largest - least * (number_of - 1)
    while spare > 0:
        free = [i for i in range(1, number_of) if given[i] < largest] or [i for i in range(1, number_of) if given[i] < most]
        pool, budget = sum([weights[i] for i in free]), spare
        for i in free:
            addition = min(most - given[i], max(1, budget * weights[i] // pool), spare)
            given[i] = given[i] + addition
            spare = spare - addition
    return np.array(given)


def bell_draw(stream_key, dims, spread, bound, split=(), held_as=jnp.bfloat16):
    factor_of = block_scale(stream_key, dims, split, -0.22, 0.18) if split else 1.0
    values = jax.random.normal(stream_key, dims, jnp.float32) * spread * factor_of
    return jnp.minimum(jnp.maximum(values, -bound), bound).astype(held_as)


def setup_inputs(seed: int = 0) -> dict:
    seeds = jax.random.split(jax.random.key(seed), 14)
    queries = draw_queries(jax.random.fold_in(seeds[13], 71), 0)
    key_vectors = draw_key_vectors(jax.random.fold_in(seeds[13], 71), 0)
    value_vectors = bell_draw(seeds[2], (SEQUENCE_TOKENS, HEAD_COUNT * HD), 1.0, 5.0, ((0, 16), (1, 16)))
    forget_totals = draw_forget_totals(jax.random.fold_in(seeds[13], 71), 0)
    head_gain = jnp.clip(1.0 + 0.18 * jax.random.normal(seeds[4], (HEAD_COUNT * HD,), jnp.float32), 0.1, 1.9)
    stream = bell_draw(seeds[5], (SEQUENCE_TOKENS, D), 1.0, 6.0, ((0, 256),))
    out_weight = bell_draw(seeds[6], (HEAD_COUNT * HD, D), (HEAD_COUNT * HD) ** -0.5, 0.125)
    norm_gain = jnp.clip(1.0 + 0.18 * jax.random.normal(seeds[7], (D,), jnp.float32), 0.1, 1.9)
    routing_keys = jax.random.split(jax.random.fold_in(seeds[8], 1), SEQUENCE_TOKENS // ROWS_DEV)
    routing_turns = jax.random.permutation(jax.random.fold_in(seeds[8], 3), SEQUENCE_TOKENS // ROWS_DEV)
    routing = jax.vmap(lambda own, number: routed_block(jax.random.fold_in(seeds[8], 2), own, number, ROWS_DEV, EXPERTS, TOP, CAP, 1))(routing_keys, routing_turns).reshape((SEQUENCE_TOKENS, TOP))
    route_weights = jnp.clip(0.2 + 0.8 * jax.random.uniform(seeds[9], (SEQUENCE_TOKENS, TOP), jnp.float32) ** block_scale(seeds[9], (SEQUENCE_TOKENS, TOP), ((0, 256),), -0.2, 0.2), 0.2, 1.0)
    gate_weight = bell_draw(seeds[10], (EXPERTS, D, FF_E), D ** -0.5, 0.125, ((0, 16), (2, 16)))
    up_weight = bell_draw(seeds[11], (EXPERTS, D, FF_E), D ** -0.5, 0.125, ((0, 16), (2, 16)))
    down_weight = bell_draw(seeds[12], (EXPERTS, FF_E, D), FF_E ** -0.5, 0.09375, ((0, 16), (1, 16)))
    return {"queries": queries, "key_vectors": key_vectors, "value_vectors": value_vectors, "forget_totals": forget_totals, "head_gain": head_gain, "stream": stream, "out_weight": out_weight, "norm_gain": norm_gain, "routing": routing, "route_weights": route_weights, "gate_weight": gate_weight, "up_weight": up_weight, "down_weight": down_weight}


def attention_rows(queries, key_vectors, value_vectors, forget_totals, head_gain):
    seq_len = queries.shape[0]
    query_block = 512 if seq_len % 512 == 0 else seq_len
    query_complete = queries.astype(jnp.float32).reshape(seq_len, HEAD_COUNT, HD)
    key_all = key_vectors.astype(jnp.float32).reshape(seq_len, HEAD_COUNT, HD)
    value_all = value_vectors.astype(jnp.float32).reshape(seq_len, HEAD_COUNT, HD)
    gate_rows = jnp.transpose(forget_totals)
    key_pos = jnp.arange(seq_len, dtype=jnp.int32)
    gain_grid = head_gain.reshape(HEAD_COUNT, 1, HD)

    def one_block(block_index):
        first_row = block_index * query_block
        query_rows = lax.dynamic_slice_in_dim(query_complete, first_row, query_block, 0)
        query_gate = lax.dynamic_slice_in_dim(gate_rows, first_row, query_block, 1)
        scores = jnp.einsum('qhd,khd->hqk', query_rows, key_all) * HD ** (-0.5) + query_gate[:, :, None] - gate_rows[:, None, :]
        query_pos = first_row + jnp.arange(query_block, dtype=jnp.int32)
        visible = (key_pos[None, :] <= query_pos[:, None])[None]
        scores = jnp.where(visible, scores, -jnp.inf)
        row_peak = lax.optimization_barrier(jnp.max(scores, axis=2, keepdims=True))
        lifted = jnp.exp(scores - row_peak)
        row_total = lax.optimization_barrier(jnp.sum(lifted, axis=2))
        rounded = lax.optimization_barrier(lifted.astype(jnp.bfloat16))
        numerator = jnp.einsum('hqk,khd->hqd', rounded.astype(jnp.float32), value_all)
        attended = numerator / row_total[:, :, None]
        inverse_rms = lax.rsqrt(lax.optimization_barrier(jnp.mean(attended * attended, axis=2, keepdims=True)) + 1e-06)
        normed = attended * inverse_rms * gain_grid
        return jnp.transpose(normed, (1, 0, 2)).reshape(query_block, HEAD_COUNT * HD).astype(jnp.bfloat16)
    block_count = seq_len // query_block
    head_out = lax.map(one_block, jnp.arange(block_count, dtype=jnp.int32))
    return head_out.reshape(seq_len, HEAD_COUNT * HD)

def expert_rows(normed_rows, routing, route_weights, gate_weight, up_weight, down_weight):
    token_count = normed_rows.shape[0]
    row_block = 128
    flat_expert = routing.reshape(-1).astype(jnp.int32)
    pair_count = flat_expert.shape[0]
    flat_token = (jnp.arange(pair_count, dtype=jnp.int32) // TOP).astype(jnp.int32)
    flat_weight = route_weights.reshape(-1)
    ordering = jnp.argsort(flat_expert, stable=True)
    sorted_expert = flat_expert[ordering]
    per_expert = lax.optimization_barrier(jnp.sum((flat_expert[:, None] == jnp.arange(EXPERTS, dtype=jnp.int32)[None, :]).astype(jnp.int32), axis=0)).astype(jnp.int32)
    padded = ((per_expert + row_block - 1) // row_block * row_block).astype(jnp.int32)
    pad_end = jnp.cumsum(padded).astype(jnp.int32)
    pad_start = (pad_end - padded).astype(jnp.int32)
    run_start = (jnp.cumsum(per_expert) - per_expert).astype(jnp.int32)
    target = (pad_start[sorted_expert] + jnp.arange(pair_count, dtype=jnp.int32) - run_start[sorted_expert]).astype(jnp.int32)
    block_count = -(-pair_count // row_block) + EXPERTS
    slot_total = block_count * row_block
    slot_token = jnp.full((slot_total,), token_count, jnp.int32).at[target].set(flat_token[ordering])
    slot_weight = jnp.zeros((slot_total,), jnp.float32).at[target].set(flat_weight[ordering])
    block_starts = (jnp.arange(block_count, dtype=jnp.int32) * row_block).astype(jnp.int32)
    block_expert = jnp.minimum(jnp.searchsorted(pad_end, block_starts, side='right').astype(jnp.int32), EXPERTS - 1).astype(jnp.int32)
    padded_rows = jnp.concatenate([normed_rows, jnp.zeros((1, normed_rows.shape[1]), normed_rows.dtype)], axis=0)[slot_token]
    units_dev = FF_E // N_TP

    def expert_block(block_args):
        block_in, expert_id = block_args
        gate_pre = jnp.dot(block_in, gate_weight[expert_id], preferred_element_type=jnp.float32)
        up_pre = jnp.dot(block_in, up_weight[expert_id], preferred_element_type=jnp.float32)
        hidden = lax.optimization_barrier((jax.nn.silu(gate_pre) * up_pre).astype(jnp.bfloat16))
        grouped_rows = jnp.transpose(hidden.reshape(row_block, N_TP, units_dev), (1, 0, 2)).astype(jnp.float32)
        down_groups = down_weight[expert_id].reshape(N_TP, units_dev, -1).astype(jnp.float32)
        partial_value = lax.optimization_barrier(jnp.einsum('gbf,gfd->gbd', grouped_rows, down_groups).astype(jnp.bfloat16))
        return lax.optimization_barrier(jnp.sum(partial_value.astype(jnp.float32), axis=0)).astype(jnp.bfloat16)
    expert_out = lax.map(expert_block, (padded_rows.reshape(block_count, row_block, -1), block_expert))
    expert_out = expert_out.reshape(slot_total, -1)
    weighted = expert_out.astype(jnp.float32) * slot_weight[:, None]
    return jax.ops.segment_sum(weighted, slot_token, num_segments=token_count + 1)[:token_count]

def reference(queries, key_vectors, value_vectors, forget_totals, head_gain, stream, out_weight, norm_gain, routing, route_weights, gate_weight, up_weight, down_weight):
    head_out = attention_rows(queries, key_vectors, value_vectors, forget_totals, head_gain)
    mixed_rows = jnp.dot(head_out, out_weight, preferred_element_type=jnp.float32)
    resid_sum = stream.astype(jnp.float32) + mixed_rows
    center = resid_sum - lax.optimization_barrier(jnp.mean(resid_sum, axis=1, keepdims=True))
    normed_rows = (center * lax.rsqrt(lax.optimization_barrier(jnp.mean(center * center, axis=1, keepdims=True)) + 1e-05) * norm_gain).astype(jnp.bfloat16)
    routed = expert_rows(normed_rows, routing, route_weights, gate_weight, up_weight, down_weight)
    return (resid_sum + routed).astype(jnp.bfloat16)
```

```python
from functools import partial

import jax
import jax.numpy as jnp
from jax import lax
from jax.experimental import pallas as pl
from jax.experimental.pallas import tpu as pltpu
from jax.sharding import PartitionSpec as P

HD = 128
TOP = 2
SIDE = 4
MESH = pl.DeviceIdType.MESH
F32 = jnp.float32
BF16 = jnp.bfloat16
LOG2E = 1.4426950408889634
HIDDEN_SCORE = -1e30


def attention_kernel(
    tp_count,
    q_ref,
    k_ref,
    v_ref,
    g_ref,
    head_gain_ref,
    stream_ref,
    norm_gain_ref,
    out_w_ref,
    resid_ref,
    normed_ref,
    kb,
    vb,
    gb,
    m_ref,
    acc_ref,
    ho,
    th,
    w_buf,
    kv_send,
    kv_recv,
    g_send,
    g_recv,
    h_send,
    h_recv,
    w_sem,
):
    tok = q_ref.shape[0]
    half = tok // 2
    rows = stream_ref.shape[0]
    sp_count = SIDE * SIDE
    me = lax.axis_index("sp")
    tpi = lax.axis_index("tp")
    mx = me % SIDE
    my = me // SIDE

    def sp_of(x, y):
        return (y % SIDE) * SIDE + x % SIDE

    fetch_w = pltpu.make_async_copy(out_w_ref, w_buf, w_sem)
    fetch_w.start()

    barrier = pltpu.get_barrier_semaphore()

    @pl.loop(1, sp_count)
    def _(j):
        pl.semaphore_signal(
            barrier, inc=1, device_id=((me + j) % sp_count, tpi), device_id_type=MESH
        )

    @pl.loop(1, tp_count)
    def _(j):
        pl.semaphore_signal(
            barrier, inc=1, device_id=(me, (tpi + j) % tp_count), device_id_type=MESH
        )

    pl.semaphore_wait(barrier, sp_count - 1 + tp_count - 1)

    def piece(ref, blk, part):
        if part is None:
            return ref.at[blk]
        return ref.at[blk, pl.ds(part * half, half), :]

    def place(kind, a, b):
        return sp_of(a, b) if kind == 0 else sp_of(b, a)

    def copy(kind, idx, block, part, target):
        buf = (kb, vb)[kind]
        own = (k_ref, v_ref)[kind]
        ma, mb = (mx, my) if kind == 0 else (my, mx)
        blk = place(kind, ma + block[0], mb + block[1])
        if block == (0, 0):
            src = own if part is None else own.at[pl.ds(part * half, half), :]
        else:
            src = piece(buf, blk, part)
        return pltpu.make_async_remote_copy(
            src_ref=src,
            dst_ref=piece(buf, blk, part),
            send_sem=kv_send.at[kind, idx],
            recv_sem=kv_recv.at[kind, idx],
            device_id=(place(kind, ma + target[0], mb + target[1]), tpi),
            device_id_type=MESH,
        )

    plan = {
        0: ((0, 0), None, (1, 0)),
        1: ((0, 0), None, (-1, 0)),
        2: ((-1, 0), 0, (1, 0)),
        3: ((1, 0), 1, (-1, 0)),
    }
    for n, a in enumerate((0, -1, 1, 2)):
        plan[4 + 4 * n] = ((a, 0), None, (0, 1))
        plan[5 + 4 * n] = ((a, 0), None, (0, -1))
        plan[6 + 4 * n] = ((a, -1), 0, (0, 1))
        plan[7 + 4 * n] = ((a, 1), 1, (0, -1))

    def send(kind, idx):
        block, part, target = plan[idx]
        copy(kind, idx, block, part, target).start()

    def arrive(kind, idx):
        block, part, target = plan[idx]
        buf = (kb, vb)[kind]
        ma, mb = (mx, my) if kind == 0 else (my, mx)
        blk = place(kind, ma + block[0] - target[0], mb + block[1] - target[1])
        pltpu.make_async_remote_copy(
            src_ref=piece(buf, blk, part),
            dst_ref=piece(buf, blk, part),
            send_sem=kv_send.at[kind, idx],
            recv_sem=kv_recv.at[kind, idx],
            device_id=(place(kind, ma + target[0], mb + target[1]), tpi),
            device_id_type=MESH,
        ).wait_recv()

    def gate_copy(j, blk_out):
        return pltpu.make_async_remote_copy(
            src_ref=g_ref,
            dst_ref=gb.at[blk_out],
            send_sem=g_send.at[j - 1],
            recv_sem=g_recv.at[j - 1],
            device_id=((me + j) % sp_count, tpi),
            device_id_type=MESH,
        )

    for idx in (0, 1):
        send(0, idx)
    for idx in (0, 1):
        send(1, idx)

    @pl.loop(1, sp_count)
    def _(j):
        gate_copy(j, me).start()

    for idx in (4, 5):
        send(0, idx)
    for idx in (4, 5):
        send(1, idx)

    scale = HD ** (-0.5) * LOG2E
    part_rows = min(256, tok)
    reps = tok // HD

    def fold(k_blk, v_blk, g_row, first):
        v_ones = jnp.concatenate([v_blk, jnp.ones((tok, HD), BF16)], axis=1)
        for r in range(tok // part_rows):
            rs = pl.ds(r * part_rows, part_rows)
            s = lax.dot_general(
                q_ref[rs, :], k_blk, (((1,), (1,)), ((), ())), preferred_element_type=F32
            )
            t = s * scale + g_row
            if first:
                keys = lax.broadcasted_iota(jnp.int32, (part_rows, tok), 1)
                qs = lax.broadcasted_iota(jnp.int32, (part_rows, tok), 0) + r * part_rows
                t = jnp.where(keys <= qs, t, HIDDEN_SCORE)
            top = jnp.max(t, axis=1, keepdims=True)
            if first:
                m_new = jnp.broadcast_to(top, (part_rows, HD))
            else:
                m_old = m_ref[rs, :]
                m_new = jnp.maximum(m_old, top)
            p = jnp.exp2(t - jnp.concatenate([m_new] * reps, axis=1))
            pv = jnp.dot(p.astype(BF16), v_ones, preferred_element_type=F32)
            if first:
                acc_ref[rs, :] = pv
            else:
                alpha = jnp.exp2(m_old - m_new)
                acc_ref[rs, :] = acc_ref[rs, :] * jnp.concatenate([alpha] * 2, axis=1) + pv
            m_ref[rs, :] = m_new

    fold(k_ref[...], v_ref[...], g_ref[...], True)

    @pl.loop(1, sp_count)
    def _(i):
        @pl.when(i == 1)
        def _():
            for kind in (0, 1):
                arrive(kind, 0)
                for idx in (2, 8, 9):
                    send(kind, idx)
                arrive(kind, 1)
                for idx in (3, 12, 13):
                    send(kind, idx)
            for kind in (0, 1):
                arrive(kind, 4)
                send(kind, 6)
                arrive(kind, 5)
                send(kind, 7)

            @pl.loop(1, sp_count)
            def _(j):
                gate_copy(j, (me + sp_count - j) % sp_count).wait_recv()

        @pl.when(i == 5)
        def _():
            for kind in (0, 1):
                arrive(kind, 2)
                arrive(kind, 3)
                for idx in (16, 17):
                    send(kind, idx)
            for kind in (0, 1):
                for got, idx in ((8, 10), (9, 11), (12, 14), (13, 15)):
                    arrive(kind, got)
                    send(kind, idx)
            for kind in (0, 1):
                arrive(kind, 6)
                arrive(kind, 7)

        @pl.when(i == 11)
        def _():
            for kind in (0, 1):
                for got, idx in ((16, 18), (17, 19)):
                    arrive(kind, got)
                    send(kind, idx)
            for kind in (0, 1):
                for got in (10, 11, 14, 15):
                    arrive(kind, got)

        @pl.when(i == 15)
        def _():
            for kind in (0, 1):
                arrive(kind, 18)
                arrive(kind, 19)

        def since(n):
            return (i + 16 - n) // 16

        j1, j2, j3, j4 = i - 1 + 16, i - 5, i - 7 + 16, i - 11 + 16
        w1 = since(1) - since(5)
        w2 = since(5) - since(7)
        w3 = since(7) - since(11)
        w4 = since(11) - since(15)
        w5 = since(15)
        h1, p1 = (j1 - 16 + 16) // 2 - 8, 1 + 2 * (j1 % 2)
        p3, q3 = 1 + 2 * (j3 % 2), 1 + 2 * (j3 // 2 - 8)
        h4, p4 = j4 // 2 - 8, 1 + 2 * (j4 % 2)
        dx = (
            w1 * (1 - h1) * p1
            + w2 * 2 * (1 - j2)
            + w3 * p3
            + w4 * ((1 - h4) * 2 + h4 * p4)
            + w5 * 2
        )
        dy = w1 * h1 * p1 + w2 * 2 * j2 + w3 * q3 + w4 * ((1 - h4) * p4 + h4 * 2) + w5 * 2
        blk = sp_of(mx + dx, my + dy)

        @pl.when(blk < me)
        def _():
            fold(kb[blk], vb[blk], gb[blk], False)

    total = acc_ref[...]
    attended = total[:, :HD] / total[:, HD:]
    rms = lax.rsqrt(jnp.mean(attended * attended, axis=1, keepdims=True) + 1e-06)
    ho[...] = (attended * rms * head_gain_ref[...]).astype(BF16)

    def head_copy(j, block):
        to = (tpi + j) % tp_count
        return pltpu.make_async_remote_copy(
            src_ref=ho.at[pl.ds(pl.multiple_of(to * rows, rows), rows), :],
            dst_ref=th.at[block],
            send_sem=h_send.at[j - 1],
            recv_sem=h_recv.at[j - 1],
            device_id=(me, to),
            device_id_type=MESH,
        )

    @pl.loop(1, tp_count)
    def _(j):
        head_copy(j, tpi).start()

    for kind in (0, 1):
        for idx in range(20):
            block, part, target = plan[idx]
            copy(kind, idx, block, part, target).wait_send()

    @pl.loop(1, sp_count)
    def _(j):
        gate_copy(j, me).wait_send()

    th[tpi] = ho[pl.ds(pl.multiple_of(tpi * rows, rows), rows), :]
    fetch_w.wait()

    @pl.loop(1, tp_count)
    def _(j):
        head_copy(j, (tpi + tp_count - j) % tp_count).wait_recv()

    heads = jnp.concatenate([th[t] for t in range(tp_count)], axis=1)
    width = out_w_ref.shape[1]
    step = min(512, width)

    @pl.loop(0, width // step)
    def _(n):
        cols = pl.ds(pl.multiple_of(n * step, step), step)
        resid_ref[:, cols] = stream_ref[:, cols].astype(F32) + jnp.dot(
            heads, w_buf[:, cols], preferred_element_type=F32
        )

    resid = resid_ref[...]
    center = resid - jnp.mean(resid, axis=1, keepdims=True)
    spread = lax.rsqrt(jnp.mean(center * center, axis=1, keepdims=True) + 1e-05)
    normed_ref[...] = (center * spread * norm_gain_ref[...]).astype(BF16)

    @pl.loop(1, tp_count)
    def _(j):
        head_copy(j, tpi).wait_send()


def attention_part(
    tp_count, queries, key_vectors, value_vectors, forget_totals, head_gain, stream, out_weight, norm_gain
):
    tok = queries.shape[0]
    rows, width = stream.shape
    sp_count = SIDE * SIDE
    gates = (forget_totals * (-LOG2E)).reshape(1, tok)
    in_vmem = pl.BlockSpec(memory_space=pltpu.VMEM)
    return pl.pallas_call(
        partial(attention_kernel, tp_count),
        name="attention",
        out_shape=(
            jax.ShapeDtypeStruct((rows, width), F32),
            jax.ShapeDtypeStruct((rows, width), BF16),
        ),
        in_specs=[in_vmem] * 7 + [pl.BlockSpec(memory_space=pl.ANY)],
        out_specs=(in_vmem, in_vmem),
        scratch_shapes=[
            pltpu.VMEM((sp_count, tok, HD), BF16),
            pltpu.VMEM((sp_count, tok, HD), BF16),
            pltpu.VMEM((sp_count, 1, tok), F32),
            pltpu.VMEM((tok, HD), F32),
            pltpu.VMEM((tok, 2 * HD), F32),
            pltpu.VMEM((tok, HD), BF16),
            pltpu.VMEM((tp_count, rows, HD), BF16),
            pltpu.VMEM(out_weight.shape, BF16),
            pltpu.SemaphoreType.DMA((2, 20)),
            pltpu.SemaphoreType.DMA((2, 20)),
            pltpu.SemaphoreType.DMA((sp_count - 1,)),
            pltpu.SemaphoreType.DMA((sp_count - 1,)),
            pltpu.SemaphoreType.DMA((tp_count - 1,)),
            pltpu.SemaphoreType.DMA((tp_count - 1,)),
            pltpu.SemaphoreType.DMA,
        ],
        compiler_params=pltpu.CompilerParams(
            collective_id=0, has_side_effects=True, vmem_limit_bytes=48 * 1024 * 1024
        ),
    )(
        queries,
        key_vectors,
        value_vectors,
        gates,
        head_gain.reshape(1, HD),
        stream,
        norm_gain.reshape(1, width),
        out_weight,
    )


def on_device(
    tp_count,
    queries,
    key_vectors,
    value_vectors,
    forget_totals,
    head_gain,
    stream,
    out_weight,
    norm_gain,
    routing,
    route_weights,
    gate_weight,
    up_weight,
    down_weight,
):
    sp_count = lax.axis_size("sp")
    resid_sum, normed_rows = attention_part(
        tp_count,
        queries,
        key_vectors,
        value_vectors,
        forget_totals,
        head_gain,
        stream,
        out_weight,
        norm_gain,
    )
    row_count = normed_rows.shape[0]
    capacity = max(2, 2 * TOP * row_count // sp_count)
    flat_expert = routing.reshape(-1)
    onehot = (flat_expert[:, None] == jnp.arange(sp_count, dtype=jnp.int32)[None, :]).astype(
        jnp.int32
    )
    earlier = jnp.cumsum(onehot, axis=0) - onehot
    slot_index = flat_expert * capacity + jnp.sum(earlier * onehot, axis=1)
    slot_grid = slot_index.reshape(row_count, TOP)
    slot_ids = jnp.arange(sp_count * capacity, dtype=jnp.int32)
    placing = jnp.sum(
        (slot_grid[None, :, :] == slot_ids[:, None, None]).astype(jnp.float32), axis=2
    ).astype(jnp.bfloat16)
    outgoing = jnp.dot(placing, normed_rows, preferred_element_type=jnp.float32).astype(
        jnp.bfloat16
    )
    outgoing = outgoing.reshape(sp_count, capacity, normed_rows.shape[1])
    arrived = lax.all_to_all(outgoing, "sp", split_axis=0, concat_axis=0, tiled=True)
    row_piece = lax.all_gather(arrived.reshape(-1, arrived.shape[2]), "tp", axis=0, tiled=True)
    gate_pre = jnp.dot(row_piece, gate_weight[0], preferred_element_type=jnp.float32)
    up_pre = jnp.dot(row_piece, up_weight[0], preferred_element_type=jnp.float32)
    hidden = (jax.nn.silu(gate_pre) * up_pre).astype(jnp.bfloat16)
    summed = lax.psum_scatter(
        jnp.dot(hidden, down_weight[0], preferred_element_type=jnp.float32).astype(jnp.bfloat16),
        "tp",
        scatter_dimension=0,
        tiled=True,
    )
    expert_out = summed.reshape(sp_count, capacity, -1)
    returned = lax.all_to_all(expert_out, "sp", split_axis=0, concat_axis=0, tiled=True)
    picked = returned.reshape(sp_count * capacity, -1)[slot_index].astype(jnp.float32)
    weighted = picked * route_weights.reshape(-1)[:, None]
    routed = jnp.sum(weighted.reshape(row_count, TOP, -1), axis=1)
    return (resid_sum + routed).astype(jnp.bfloat16)


def solution(mesh):
    in_specs = (
        P("sp", "tp"),
        P("sp", "tp"),
        P("sp", "tp"),
        P("sp", "tp"),
        P("tp"),
        P(("sp", "tp"), None),
        P(),
        P(),
        P(("sp", "tp"), None),
        P(("sp", "tp"), None),
        P("sp", None, "tp"),
        P("sp", None, "tp"),
        P("sp", "tp", None),
    )
    out_specs = P(("sp", "tp"), None)
    return jax.shard_map(
        partial(on_device, mesh.shape["tp"]),
        mesh=mesh,
        in_specs=in_specs,
        out_specs=out_specs,
        check_vma=False,
    )
```
